32 devices in a mesh: tp: 8 (over z, y), dp: 4 (over x, core).
Axes of the slice: x: 2, y: 2, z: 4, core: 2. Of those that a mesh axis runs over, the one named last changes fastest.
Arguments:
- hidden: bfloat16 [96, 4096], P(None, 'dp'), may hold values from -14 to 14
- lengths: int32 [96], P('dp'), may hold values from 1 to 8192, 196608 in all
- norm_gain: float32 [2, 4096], P(None, 'dp'), may hold values from 0.1 to 1.9
- gate_proj: bfloat16 [2, 4096, 4096], P(None, 'dp', 'tp'), may hold values from -0.09375 to 0.09375
- input_proj: bfloat16 [2, 4096, 4096], P(None, 'dp', 'tp'), may hold values from -0.09375 to 0.09375
- coupling_proj: bfloat16 [2, 4096, 2, 2048], P(None, 'dp', None, 'tp'), may hold values from -0.09375 to 0.09375
- step_proj: bfloat16 [2, 4096, 64], P(None, 'dp'), may hold values from -0.09375 to 0.09375
- input_taps: float32 [2, 5, 4096], P(None, None, 'tp'), may hold values from -2.5 to 2.5
- coupling_taps: float32 [2, 5, 2, 2048], P(None, None, None, 'tp'), may hold values from -2.5 to 2.5
- step_bias: float32 [2, 64], replicated, may hold values from -5 to -1
- decay_log: float32 [2, 64], replicated, may hold values from -1 to 2.5
- skip_gain: float32 [2, 64], replicated, may hold values from 0.1 to 3
- span_bias: float32 [2, 8, 64], replicated, may hold values from -2 to 2
- mix_gain: float32 [2, 4096], P(None, 'tp'), may hold values from 0.1 to 1.9
- out_proj: bfloat16 [2, 4096, 4096], P(None, 'tp', 'dp'), may hold values from -0.09375 to 0.09375
- recurrent: float32 [2, 96, 64, 64, 128], P(None, 'dp', 'tp'), may hold values from -1.2 to 1.2
- input_history: bfloat16 [2, 96, 4, 4096], P(None, 'dp', None, 'tp'), may hold values from -6 to 6
- coupling_history: bfloat16 [2, 96, 4, 2, 2048], P(None, 'dp', None, None, 'tp'), may hold values from -6 to 6
Outputs:
- out_hidden: bfloat16 [96, 4096], P(None, 'dp')
- new_recurrent: float32 [2, 96, 64, 64, 128], P(None, 'dp', 'tp')
- next_inputs: bfloat16 [2, 96, 4, 4096], P(None, 'dp', None, 'tp')
- next_couplings: bfloat16 [2, 96, 4, 2, 2048], P(None, 'dp', None, None, 'tp')
The draws below stay inside these ranges and needn't reach their ends.
Inputs may be any that keep to these rules, and one draw needn't show every extreme that they name: `lengths`: every sequence's length; the longest is exactly 8192, and they sum to 2048 times the number of sequences.
All inputs are finite; a program needn't handle non-finite values. No bound on the sum of `lengths` on one device may be relied on, other than what follows from the above.
Results may differ from the reference program's by a relative error of at most 0.02.
Values may be sent and summed in bfloat16 or wider, within the bound.
A program may use at most 128 MiB of HBM per device.

```python
import math
import jax
import jax.numpy as jnp
import numpy as np
from jax import lax

D = 4096
HEADS = 64
HEAD_DIM = 64
GROUPS = 16
STATE = 128
TAPS = 5
LAYERS = 2
SPAN_LEN = 1024
MEAN_LEN = 2048
MOST_LEN = 8192
SEQ_DEV = 24
INNER = 4096
SPANS = 8
BATCH = 96
N_DP = 4


def draw_hidden(key, part):
    value_key, scale_key = jax.random.split(jax.random.fold_in(key, 17))
    scales = jnp.exp(jax.random.uniform(scale_key, (BATCH, D // 64, 1), jnp.float32, -1.2, 1.2))
    values = jnp.clip(jax.random.normal(value_key, (BATCH, D // 64, 64), jnp.float32), -4.0, 4.0)
    return (values * scales).reshape(BATCH, D).astype(jnp.bfloat16)


def levels(key, shape, pieces, low, largest):
    loudness = 1.0
    for dim, parts in pieces:
        heights = jax.random.uniform(jax.random.fold_in(jax.random.fold_in(key, 6), dim), (parts,), jnp.float32, low / len(pieces), largest / len(pieces))
        loudness = loudness * jnp.repeat(jnp.exp(heights), shape[dim] // parts).reshape((-1,) + (1,) * (len(shape) - 1 - dim))
    return loudness


def length_profile(number_of, total, reach, skew):
    loads = [(1 << 20) // math.isqrt(standing ** skew) + 1 for standing in range(2, number_of + 1)]
    rest, given = total - reach - (number_of - 1), [1] * (number_of - 1)
    while rest > 0:
        movable = [i for i in range(number_of - 1) if given[i] < reach]
        pool, budget = sum([loads[i] for i in movable]), rest
        for i in movable:
            addition = min(reach - given[i], max(1, budget * loads[i] // pool), rest)
            given[i] = given[i] + addition
            rest = rest - addition
    return np.array([reach] + given)


def uneven(key, amount, total, bound, lean):
    if amount == 2:
        one = jax.random.randint(key, (), max(1, total - bound), min(bound, total - 1) + 1)
        return jnp.stack([one, total - one])
    sizes = jnp.asarray(length_profile(amount, total, bound, lean), jnp.int32)
    pairs = (amount - 1) // 2
    donor, receiver = sizes[1:1 + 2 * pairs:2], sizes[2:2 + 2 * pairs:2]
    room = jnp.minimum(donor - 1, bound - receiver)
    moved = jax.random.randint(jax.random.fold_in(key, 1), (pairs,), 0, 1 << 20) % (room + 1)
    sizes = sizes.at[1:1 + 2 * pairs:2].set(donor - moved).at[2:2 + 2 * pairs:2].set(receiver + moved)
    return sizes[jax.random.permutation(jax.random.fold_in(key, 2), amount)]


def bell_draw(key, dims, width, bound, cuts=(), kind=jnp.bfloat16):
    array = width * jax.random.normal(key, dims, jnp.float32)
    if cuts:
        array = array * levels(key, dims, cuts, -0.22, 0.18)
    return jnp.clip(array, -bound, bound).astype(kind)


def setup_inputs(seed: int = 0) -> dict:
    splits = jax.random.split(jax.random.key(seed), 19)
    hidden = draw_hidden(jax.random.fold_in(splits[18], 71), 0)
    lengths = uneven(splits[1], BATCH, SEQ_DEV * N_DP * MEAN_LEN, MOST_LEN, 2).astype(jnp.int32)
    norm_gain = jnp.clip(1.0 + 0.18 * jax.random.normal(splits[2], (LAYERS, D), jnp.float32), 0.1, 1.9)
    gate_proj = bell_draw(splits[3], (LAYERS, D, INNER), D ** -0.5, 0.09375, ((1, 4), (2, 8)))
    input_proj = bell_draw(splits[4], (LAYERS, D, INNER), D ** -0.5, 0.09375, ((1, 4), (2, 8)))
    coupling_proj = bell_draw(splits[5], (LAYERS, D, 2, GROUPS * STATE), D ** -0.5, 0.09375, ((1, 4), (3, 8)))
    step_proj = bell_draw(splits[6], (LAYERS, D, HEADS), D ** -0.5, 0.09375, ((1, 4),))
    input_taps = bell_draw(splits[7], (LAYERS, TAPS, INNER), TAPS ** -0.5, 2.5, ((2, 8),), jnp.float32)
    coupling_taps = bell_draw(splits[8], (LAYERS, TAPS, 2, GROUPS * STATE), TAPS ** -0.5, 2.5, ((3, 8),), jnp.float32)
    step_bias = jnp.clip(jax.random.uniform(splits[9], (LAYERS, HEADS), jnp.float32, -5.0, -1.0), -5.0, -1.0)
    decay_log = jnp.clip(jax.random.uniform(splits[10], (LAYERS, HEADS), jnp.float32, -1.0, 2.5), -1.0, 2.5)
    skip_gain = jnp.clip(jnp.exp(jax.random.uniform(splits[11], (LAYERS, HEADS), jnp.float32, math.log(0.1), math.log(3.0))), 0.1, 3.0)
    span_bias = jnp.clip(jax.random.uniform(splits[12], (LAYERS, SPANS, HEADS), jnp.float32, -2.0, 2.0), -2.0, 2.0)
    mix_gain = jnp.clip(1.0 + 0.18 * jax.random.normal(splits[13], (LAYERS, INNER), jnp.float32), 0.1, 1.9)
    out_proj = bell_draw(splits[14], (LAYERS, INNER, D), INNER ** -0.5, 0.09375, ((1, 8), (2, 4)))
    recurrent = bell_draw(splits[15], (LAYERS, BATCH, HEADS, HEAD_DIM, STATE), 0.2, 1.2, ((1, 4), (2, 8)), jnp.float32)
    input_history = bell_draw(splits[16], (LAYERS, BATCH, TAPS - 1, INNER), 1.0, 6.0, ((1, 4), (3, 8)))
    coupling_history = bell_draw(splits[17], (LAYERS, BATCH, TAPS - 1, 2, GROUPS * STATE), 1.0, 6.0, ((1, 4), (4, 8)))
    return dict(hidden=hidden, lengths=lengths, norm_gain=norm_gain, gate_proj=gate_proj, input_proj=input_proj, coupling_proj=coupling_proj, step_proj=step_proj, input_taps=input_taps, coupling_taps=coupling_taps, step_bias=step_bias, decay_log=decay_log, skip_gain=skip_gain, span_bias=span_bias, mix_gain=mix_gain, out_proj=out_proj, recurrent=recurrent, input_history=input_history, coupling_history=coupling_history)


EPS = 1e-06

def norm_rows(rows, gain):
    values = rows.astype(jnp.float32)
    squares = lax.optimization_barrier(jnp.sum(values * values, axis=1))
    return (values * lax.rsqrt(squares / D + EPS)[:, None] * gain[None, :]).astype(jnp.bfloat16)

def project_rows(normed, weight):
    block_width = D // N_DP
    sum_total = jnp.zeros((normed.shape[0], weight.shape[1]), jnp.float32)
    for block_index in range(N_DP):
        low = block_index * block_width
        partial_sum = jnp.dot(normed[:, low:low + block_width], weight[low:low + block_width], preferred_element_type=jnp.float32)
        rounded = lax.optimization_barrier(partial_sum.astype(jnp.bfloat16))
        sum_total = sum_total + rounded.astype(jnp.float32)
    return lax.optimization_barrier(sum_total.astype(jnp.bfloat16))

def state_row(row_inputs):
    prior_row, decay_row, drive_row, write_row, read_row = row_inputs
    fresh_row = decay_row[:, :, None, None] * prior_row + drive_row[:, :, :, None] * write_row[:, None, None, :]
    readout_row = jnp.einsum('grpn,gn->grp', fresh_row, read_row, precision=lax.Precision.HIGHEST)
    return (fresh_row, readout_row)

def reference(hidden, lengths, norm_gain, gate_proj, input_proj, coupling_proj, step_proj, input_taps, coupling_taps, step_bias, decay_log, skip_gain, span_bias, mix_gain, out_proj, recurrent, input_history, coupling_history):
    batch_rows = hidden.shape[0]
    per_group = HEADS // GROUPS
    span_index = (lengths - 1) // SPAN_LEN
    onehot = (span_index[:, None] == jnp.arange(SPANS, dtype=jnp.int32)[None, :]).astype(jnp.float32)
    stream = hidden
    normed = norm_rows(hidden, norm_gain[0])
    states, inputs_next, couplings_next = ([], [], [])
    for layer_index in range(LAYERS):
        gate_in = project_rows(normed, gate_proj[layer_index])
        input_in = project_rows(normed, input_proj[layer_index])
        coupling_flat = project_rows(normed, coupling_proj[layer_index].reshape(D, 2 * GROUPS * STATE))
        coupling_in = coupling_flat.reshape(batch_rows, 2, GROUPS * STATE)
        step_in = project_rows(normed, step_proj[layer_index])
        input_window = jnp.concatenate([input_history[layer_index], input_in[:, None, :]], axis=1)
        coupling_window = jnp.concatenate([coupling_history[layer_index], coupling_in[:, None]], axis=1)
        inputs_next.append(input_window[:, 1:])
        couplings_next.append(coupling_window[:, 1:])
        input_act = jax.nn.silu(lax.optimization_barrier(jnp.sum(input_window.astype(jnp.float32) * input_taps[layer_index][None], axis=1)))
        coupling_act = jax.nn.silu(lax.optimization_barrier(jnp.sum(coupling_window.astype(jnp.float32) * coupling_taps[layer_index][None], axis=1)))
        span_term = lax.optimization_barrier(jnp.sum(onehot[:, :, None] * span_bias[layer_index][None], axis=1))
        step_size = jax.nn.softplus(step_in.astype(jnp.float32) + step_bias[layer_index][None] + span_term)
        decay_rate = jnp.exp(-step_size * jnp.exp(decay_log[layer_index])[None])
        input_heads = input_act.reshape(batch_rows, GROUPS, per_group, HEAD_DIM)
        write_vec = coupling_act[:, 0].reshape(batch_rows, GROUPS, STATE)
        read_vec = coupling_act[:, 1].reshape(batch_rows, GROUPS, STATE)
        drive = step_size.reshape(batch_rows, GROUPS, per_group)[..., None] * input_heads
        prior_state = recurrent[layer_index].reshape(batch_rows, GROUPS, per_group, HEAD_DIM, STATE)
        fresh_state, readout = lax.map(state_row, (prior_state, decay_rate.reshape(batch_rows, GROUPS, per_group), drive, write_vec, read_vec))
        states.append(fresh_state.reshape(batch_rows, HEADS, HEAD_DIM, STATE))
        readout = readout + skip_gain[layer_index].reshape(1, GROUPS, per_group, 1) * input_heads
        gated_out = readout.reshape(batch_rows, INNER) * jax.nn.silu(gate_in.astype(jnp.float32))
        squares = lax.optimization_barrier(jnp.sum(gated_out * gated_out, axis=1))
        mixed = (gated_out * lax.rsqrt(squares / INNER + EPS)[:, None] * mix_gain[layer_index][None]).astype(jnp.bfloat16)
        update = jnp.dot(mixed, out_proj[layer_index], preferred_element_type=jnp.float32)
        stream = (stream.astype(jnp.float32) + update).astype(jnp.bfloat16)
        if layer_index + 1 < LAYERS:
            normed = norm_rows(stream, norm_gain[layer_index + 1])
    return (stream, jnp.stack(states), jnp.stack(inputs_next), jnp.stack(couplings_next))
```

```python
import functools

import jax
import jax.numpy as jnp
from jax import lax
from jax.experimental import pallas as pl
from jax.experimental.pallas import tpu as pltpu
from jax.sharding import PartitionSpec as P

HEAD_DIM = 64
STATE = 128
LAYERS = 2
SPAN_LEN = 1024
SPANS = 8
LANES = 128
ROWS = 8
EPS = 1e-06
VMEM_LIMIT = 40 * 1024 * 1024
MESH = pl.DeviceIdType.MESH
F32 = jnp.float32
BF16 = jnp.bfloat16


def head_slice(param_table, take_count):
    return lax.dynamic_slice_in_dim(
        param_table, lax.axis_index("tp") * take_count, take_count, param_table.ndim - 1
    )


def greet(axes):
    barrier = pltpu.get_barrier_semaphore()
    total = 0
    for axis, count in axes:
        me = lax.axis_index(axis)
        for k in range(1, count):
            pl.semaphore_signal(
                barrier, inc=1, device_id={axis: lax.rem(me + k, count)}, device_id_type=MESH
            )
            total += 1
    pl.semaphore_wait(barrier, total)


def remote(src, dst, send_sem, recv_sem, axis, peer):
    return pltpu.make_async_remote_copy(
        src_ref=src,
        dst_ref=dst,
        send_sem=send_sem,
        recv_sem=recv_sem,
        device_id={axis: peer},
        device_id_type=MESH,
    )


def split_sum(squares, width=LANES):
    high = squares.astype(BF16).astype(F32)
    low = squares - high
    lane = lax.broadcasted_iota(jnp.int32, (squares.shape[0], width), 1)
    return jnp.where(lane == 0, high, jnp.where(lane == 1, low, 0.0))


def project_kernel(
    n_dp, rows, features, x_ref, gain_ref, gate_ref, input_ref, coup_ref, step_ref,
    out_ref, send_buf, recv_buf, send_sem, recv_sem,
):
    me = lax.axis_index("dp")
    greet((("dp", n_dp),))
    values = x_ref[...].astype(F32)
    squares = jnp.sum(values * values, axis=1, keepdims=True)
    scaled = (values * gain_ref[...]).astype(BF16)

    def put(first, block):
        for d in range(n_dp):
            send_buf[d, :, first:first + block.shape[1]] = block[d * rows:(d + 1) * rows].astype(BF16)

    first = 0
    for ref in (gate_ref, input_ref, coup_ref):
        weight = ref[0] if len(ref.shape) == 3 else ref[...]
        put(first, jnp.dot(scaled, weight, preferred_element_type=F32))
        first += weight.shape[1]
    steps = lax.dot_general(
        scaled, step_ref[0], (((1,), (1,)), ((), ())), preferred_element_type=F32
    )
    spare = -steps.shape[1] % LANES
    if spare:
        steps = jnp.concatenate([steps, jnp.zeros((steps.shape[0], spare), F32)], axis=1)
    put(first, steps)
    first += steps.shape[1]
    put(first, split_sum(squares))

    copies = []
    for k in range(1, n_dp):
        peer = lax.rem(me + k, n_dp)
        copy = remote(
            send_buf.at[peer], recv_buf.at[k - 1], send_sem.at[k - 1], recv_sem.at[k - 1], "dp", peer
        )
        copy.start()
        copies.append(copy)
    total = send_buf[me].astype(F32)
    for k in range(1, n_dp):
        copies[k - 1].wait_recv()
        total = total + recv_buf[k - 1].astype(F32)
    squares = total[:, first:first + 1] + total[:, first + 1:first + 2]
    out_ref[...] = total[:, :first] * lax.rsqrt(squares / features + EPS)
    for copy in copies:
        copy.wait_send()


def state_kernel(
    heads, per_group, drive_ref, decay_ref, write_ref, read_ref, skip_ref, gate_ref, gain_ref,
    prior_ref, *rest,
):
    fresh_ref, gated_ref = rest[-2], rest[-1]
    drive_t = jnp.transpose(drive_ref[...])
    lane = lax.broadcasted_iota(jnp.int32, (HEAD_DIM, LANES), 1)
    sums = [jnp.zeros((HEAD_DIM, LANES), F32) for _ in range(heads)]
    for j in range(ROWS):
        for h in range(heads):
            g = h // per_group
            write = write_ref[j:j + 1, g * STATE:(g + 1) * STATE]
            read = read_ref[j:j + 1, g * STATE:(g + 1) * STATE]
            column = drive_t[h * HEAD_DIM:(h + 1) * HEAD_DIM, j:j + 1]
            fresh = decay_ref[j, h:h + 1, :] * prior_ref[0, j, h] + column * write
            fresh_ref[0, j, h] = fresh
            total = jnp.sum(fresh * read, axis=1, keepdims=True)
            sums[h] = jnp.where(lane == j, total, sums[h])
    readout = jnp.transpose(jnp.concatenate(sums, axis=0))[:ROWS]
    gated = (readout + skip_ref[...]) * gate_ref[...]
    squares = jnp.sum(gated * gated, axis=1, keepdims=True)
    inner = gated.shape[1]
    gated_ref[:, :inner] = gated * gain_ref[...]
    gated_ref[:, inner:] = split_sum(squares)


def output_kernel(
    n_dp, n_tp, rows, share, inner, gated_ref, weight_ref, stream_ref, out_ref,
    mine_buf, gather_buf, part_buf, sum_buf, row_buf,
    dp_send, dp_recv, rs_send, rs_recv, ag_send, ag_recv,
):
    dp, tp = lax.axis_index("dp"), lax.axis_index("tp")
    local = weight_ref.shape[1]
    width = weight_ref.shape[2]
    greet((("dp", n_dp), ("tp", n_tp)))
    mine_buf[...] = gated_ref[...].astype(BF16)
    gathers = []
    for k in range(1, n_dp):
        copy = remote(
            mine_buf, gather_buf.at[k - 1], dp_send.at[k - 1], dp_recv.at[k - 1], "dp",
            lax.rem(dp + k, n_dp),
        )
        copy.start()
        gathers.append(copy)

    per_dp = rows // share

    def product(block, owner):
        part = jnp.dot(block[:, :local], weight_ref[0], preferred_element_type=F32)
        for s in range(per_dp):
            slot = owner * per_dp + s
            part_buf[slot, :, :width] = part[s * share:(s + 1) * share].astype(BF16)
            part_buf[slot, :, width:] = block[s * share:(s + 1) * share, local:]

    product(mine_buf[...], dp)
    for k in range(1, n_dp):
        gathers[k - 1].wait_recv()
        product(gather_buf[k - 1], lax.rem(dp + n_dp - k, n_dp))
    scatters = []
    for k in range(1, n_tp):
        peer = lax.rem(tp + k, n_tp)
        copy = remote(
            part_buf.at[peer], sum_buf.at[k - 1], rs_send.at[k - 1], rs_recv.at[k - 1], "tp", peer
        )
        copy.start()
        scatters.append(copy)
    total = part_buf[tp].astype(F32)
    for k in range(1, n_tp):
        scatters[k - 1].wait_recv()
        total = total + sum_buf[k - 1].astype(F32)
    squares = total[:, width:width + 1] + total[:, width + 1:width + 2]
    update = total[:, :width] * lax.rsqrt(squares / inner + EPS)
    row_buf[tp] = (stream_ref[tp].astype(F32) + update).astype(BF16)
    spreads = []
    for k in range(1, n_tp):
        copy = remote(
            row_buf.at[tp], row_buf.at[tp], ag_send.at[k - 1], ag_recv.at[k - 1], "tp",
            lax.rem(tp + k, n_tp),
        )
        copy.start()
        spreads.append(copy)
    out_ref[tp] = row_buf[tp]
    for k in range(1, n_tp):
        source = lax.rem(tp + n_tp - k, n_tp)
        remote(
            row_buf.at[source], row_buf.at[source], ag_send.at[k - 1], ag_recv.at[k - 1], "tp", source
        ).wait_recv()
        out_ref[source] = row_buf[source]
    for copy in gathers + scatters + spreads:
        copy.wait_send()


def whole(shape):
    return pl.BlockSpec(shape, lambda i: (0,) * len(shape))


def of_layer(shape, layer):
    return pl.BlockSpec((1,) + shape[1:], lambda i: (layer,) + (0,) * (len(shape) - 1))


def project(layer, n_dp, stream, gain, gate, inputs, coupling, steps):
    batch, width = stream.shape
    rows = batch // n_dp
    step_lanes = -(-steps.shape[1] // LANES) * LANES
    columns = gate.shape[2] + inputs.shape[2] + coupling.shape[1] + step_lanes
    return pl.pallas_call(
        functools.partial(project_kernel, n_dp, rows, width * n_dp),
        grid=(1,),
        out_shape=jax.ShapeDtypeStruct((rows, columns), F32),
        in_specs=[
            whole(stream.shape),
            whole(gain.shape),
            of_layer(gate.shape, layer),
            of_layer(inputs.shape, layer),
            whole(coupling.shape),
            of_layer(steps.shape, layer),
        ],
        out_specs=whole((rows, columns)),
        scratch_shapes=[
            pltpu.VMEM((n_dp, rows, columns + LANES), BF16),
            pltpu.VMEM((n_dp - 1, rows, columns + LANES), BF16),
            pltpu.SemaphoreType.DMA((n_dp - 1,)),
            pltpu.SemaphoreType.DMA((n_dp - 1,)),
        ],
        compiler_params=pltpu.CompilerParams(
            collective_id=2 * layer, has_side_effects=True, vmem_limit_bytes=VMEM_LIMIT
        ),
    )(stream, gain, gate, inputs, coupling, steps)


def advance(layer, per_group, drive, decay, write, read, skip, gate, gain, recurrent, held):
    count, inner = drive.shape
    heads = recurrent.shape[2]

    def strip(width):
        return pl.BlockSpec((ROWS, width), lambda i: (i, 0))

    state_spec = pl.BlockSpec(
        (1, ROWS) + recurrent.shape[2:], lambda i: (layer, i, 0, 0, 0)
    )
    in_specs = [
        strip(inner),
        pl.BlockSpec((ROWS, heads, LANES), lambda i: (i, 0, 0)),
        strip(write.shape[1]),
        strip(read.shape[1]),
        strip(inner),
        strip(inner),
        whole(gain.shape),
        state_spec,
    ]
    operands = [drive, decay, write, read, skip, gate, gain, recurrent]
    aliases = {}
    if held is not None:
        aliases = {len(operands): 0}
        operands.append(held)
        in_specs.append(pl.BlockSpec(memory_space=pl.ANY))
    return pl.pallas_call(
        functools.partial(state_kernel, heads, per_group),
        grid=(count // ROWS,),
        out_shape=(
            jax.ShapeDtypeStruct(recurrent.shape, F32),
            jax.ShapeDtypeStruct((count, inner + LANES), F32),
        ),
        in_specs=in_specs,
        out_specs=(state_spec, strip(inner + LANES)),
        input_output_aliases=aliases,
        compiler_params=pltpu.CompilerParams(vmem_limit_bytes=VMEM_LIMIT),
    )(*operands)


def output(layer, n_dp, n_tp, gated, weight, stream):
    rows = gated.shape[0]
    share, width = stream.shape[1:]
    return pl.pallas_call(
        functools.partial(output_kernel, n_dp, n_tp, rows, share, weight.shape[1] * n_tp),
        grid=(1,),
        out_shape=jax.ShapeDtypeStruct(stream.shape, BF16),
        in_specs=[whole(gated.shape), of_layer(weight.shape, layer), whole(stream.shape)],
        out_specs=whole(stream.shape),
        scratch_shapes=[
            pltpu.VMEM(gated.shape, BF16),
            pltpu.VMEM((n_dp - 1,) + gated.shape, BF16),
            pltpu.VMEM((n_tp, share, width + LANES), BF16),
            pltpu.VMEM((n_tp - 1, share, width + LANES), BF16),
            pltpu.VMEM(stream.shape, BF16),
            pltpu.SemaphoreType.DMA((n_dp - 1,)),
            pltpu.SemaphoreType.DMA((n_dp - 1,)),
            pltpu.SemaphoreType.DMA((n_tp - 1,)),
            pltpu.SemaphoreType.DMA((n_tp - 1,)),
            pltpu.SemaphoreType.DMA((n_tp - 1,)),
            pltpu.SemaphoreType.DMA((n_tp - 1,)),
        ],
        compiler_params=pltpu.CompilerParams(
            collective_id=2 * layer + 1, has_side_effects=True, vmem_limit_bytes=VMEM_LIMIT
        ),
    )(gated, weight, stream)


def on_device(
    hidden,
    lengths,
    norm_gain,
    gate_proj,
    input_proj,
    coupling_proj,
    step_proj,
    input_taps,
    coupling_taps,
    step_bias,
    decay_log,
    skip_gain,
    span_bias,
    mix_gain,
    out_proj,
    recurrent,
    input_history,
    coupling_history,
):
    n_dp, n_tp = lax.axis_size("dp"), lax.axis_size("tp")
    batch, width = hidden.shape
    share = batch // n_tp
    rows, heads = recurrent.shape[1:3]
    inner = gate_proj.shape[2]
    groups = coupling_proj.shape[3] // STATE
    per_group = heads // groups
    half = groups * STATE
    steps_t = jnp.swapaxes(step_proj, 1, 2)
    span_index = (lengths - 1) // SPAN_LEN
    onehot = (span_index[:, None] == jnp.arange(SPANS, dtype=jnp.int32)[None, :]).astype(F32)
    stream = hidden.reshape(n_tp, share, width)
    states = None
    inputs_next, couplings_next = [], []
    for l in range(LAYERS):
        coupling = coupling_proj[l].reshape(width, 2 * half)
        sums = project(
            l, n_dp, stream.reshape(batch, width), norm_gain[l:l + 1], gate_proj, input_proj,
            coupling, steps_t,
        )
        gate_in = sums[:, :inner].astype(BF16)
        input_in = sums[:, inner:2 * inner].astype(BF16)
        coupling_in = sums[:, 2 * inner:2 * inner + 2 * half].astype(BF16).reshape(rows, 2, half)
        step_in = head_slice(sums[:, 2 * inner + 2 * half:][:, :step_proj.shape[2]], heads)
        step_in = step_in.astype(BF16)
        input_window = jnp.concatenate([input_history[l], input_in[:, None, :]], axis=1)
        coupling_window = jnp.concatenate([coupling_history[l], coupling_in[:, None]], axis=1)
        inputs_next.append(input_window[:, 1:])
        couplings_next.append(coupling_window[:, 1:])
        input_act = jax.nn.silu(jnp.sum(input_window.astype(F32) * input_taps[l][None], axis=1))
        coupling_act = jax.nn.silu(
            jnp.sum(coupling_window.astype(F32) * coupling_taps[l][None], axis=1)
        )
        span_term = jnp.sum(onehot[:, :, None] * head_slice(span_bias[l], heads)[None], axis=1)
        step_size = jax.nn.softplus(
            step_in.astype(F32) + head_slice(step_bias[l], heads)[None] + span_term
        )
        decay = jnp.exp(-step_size * jnp.exp(head_slice(decay_log[l], heads))[None])
        heads_in = input_act.reshape(rows, heads, HEAD_DIM)
        drive = (step_size[:, :, None] * heads_in).reshape(rows, inner)
        skip = (head_slice(skip_gain[l], heads)[None, :, None] * heads_in).reshape(rows, inner)
        states, gated = advance(
            l,
            per_group,
            drive,
            jnp.broadcast_to(decay[:, :, None], (rows, heads, LANES)),
            coupling_act[:, 0],
            coupling_act[:, 1],
            skip,
            jax.nn.silu(gate_in.astype(F32)),
            mix_gain[l:l + 1],
            recurrent,
            states,
        )
        stream = output(l, n_dp, n_tp, gated, out_proj, stream)
    return (
        stream.reshape(batch, width),
        states,
        jnp.stack(inputs_next),
        jnp.stack(couplings_next),
    )


def solution(mesh):
    placed = (
        P(None, "dp"),
        P("dp"),
        P(None, "dp"),
        P(None, "dp", "tp"),
        P(None, "dp", "tp"),
        P(None, "dp", None, "tp"),
        P(None, "dp", None),
        P(None, None, "tp"),
        P(None, None, None, "tp"),
        P(),
        P(),
        P(),
        P(),
        P(None, "tp"),
        P(None, "tp", "dp"),
        P(None, "dp", "tp", None, None),
        P(None, "dp", None, "tp"),
        P(None, "dp", None, None, "tp"),
    )
    return jax.shard_map(
        on_device,
        mesh=mesh,
        in_specs=placed,
        out_specs=(
            P(None, "dp"),
            P(None, "dp", "tp", None, None),
            P(None, "dp", None, "tp"),
            P(None, "dp", None, None, "tp"),
        ),
        check_vma=False,
    )
```

```python
import functools

import jax
import jax.numpy as jnp
from jax import lax
from jax.experimental import pallas as pl
from jax.experimental.pallas import tpu as pltpu
from jax.sharding import PartitionSpec as P

HEAD_DIM = 64
STATE = 128
LAYERS = 2
SPAN_LEN = 1024
SPANS = 8
LANES = 128
ROWS = 8
EPS = 1e-06
VMEM_LIMIT = 60 * 1024 * 1024
MESH = pl.DeviceIdType.MESH
F32 = jnp.float32
BF16 = jnp.bfloat16


def head_slice(param_table, take_count):
    return lax.dynamic_slice_in_dim(
        param_table, lax.axis_index("tp") * take_count, take_count, param_table.ndim - 1
    )


def greet(axes):
    barrier = pltpu.get_barrier_semaphore()
    total = 0
    for axis, count in axes:
        me = lax.axis_index(axis)
        for k in range(1, count):
            pl.semaphore_signal(
                barrier, inc=1, device_id={axis: lax.rem(me + k, count)}, device_id_type=MESH
            )
            total += 1
    pl.semaphore_wait(barrier, total)


def remote(src, dst, send_sem, recv_sem, axis, peer):
    return pltpu.make_async_remote_copy(
        src_ref=src,
        dst_ref=dst,
        send_sem=send_sem,
        recv_sem=recv_sem,
        device_id={axis: peer},
        device_id_type=MESH,
    )


def split_sum(squares, width=LANES):
    high = squares.astype(BF16).astype(F32)
    low = squares - high
    lane = lax.broadcasted_iota(jnp.int32, (squares.shape[0], width), 1)
    return jnp.where(lane == 0, high, jnp.where(lane == 1, low, 0.0))


def project_kernel(
    n_dp, rows, features, layer, x_ref, gain_ref, gate_ref, input_ref, coup_ref, step_ref,
    out_ref, gate_buf, input_buf, coup_buf, send_buf, recv_buf, load_sem, send_sem, recv_sem,
):
    me = lax.axis_index("dp")
    loads = [
        pltpu.make_async_copy(gate_ref.at[layer], gate_buf, load_sem.at[0]),
        pltpu.make_async_copy(input_ref.at[layer], input_buf, load_sem.at[1]),
        pltpu.make_async_copy(coup_ref, coup_buf, load_sem.at[2]),
    ]
    for load in loads:
        load.start()
    greet((("dp", n_dp),))
    values = x_ref[...].astype(F32)
    squares = jnp.sum(values * values, axis=1, keepdims=True)
    scaled = (values * gain_ref[...]).astype(BF16)

    def put(first, block):
        for d in range(n_dp):
            send_buf[d, :, first:first + block.shape[1]] = block[d * rows:(d + 1) * rows].astype(BF16)

    first = 0
    for load, buf in zip(loads, (gate_buf, input_buf, coup_buf)):
        load.wait()
        put(first, jnp.dot(scaled, buf[...], preferred_element_type=F32))
        first += buf.shape[1]
    steps = lax.dot_general(
        scaled, step_ref[0], (((1,), (1,)), ((), ())), preferred_element_type=F32
    )
    spare = -steps.shape[1] % LANES
    if spare:
        steps = jnp.concatenate([steps, jnp.zeros((steps.shape[0], spare), F32)], axis=1)
    put(first, steps)
    first += steps.shape[1]
    put(first, split_sum(squares))

    copies = []
    for k in range(1, n_dp):
        peer = lax.rem(me + k, n_dp)
        copy = remote(
            send_buf.at[peer], recv_buf.at[k - 1], send_sem.at[k - 1], recv_sem.at[k - 1], "dp", peer
        )
        copy.start()
        copies.append(copy)
    total = send_buf[me].astype(F32)
    for k in range(1, n_dp):
        copies[k - 1].wait_recv()
        total = total + recv_buf[k - 1].astype(F32)
    squares = total[:, first:first + 1] + total[:, first + 1:first + 2]
    out_ref[...] = total[:, :first] * lax.rsqrt(squares / features + EPS)
    for copy in copies:
        copy.wait_send()


def state_kernel(
    heads, per_group, drive_ref, decay_ref, write_ref, read_ref, skip_ref, gate_ref, gain_ref,
    prior_ref, *rest,
):
    fresh_ref, gated_ref = rest[-2], rest[-1]
    drive_t = jnp.transpose(drive_ref[...])
    groups = heads // per_group
    lane = lax.broadcasted_iota(jnp.int32, (per_group * HEAD_DIM, LANES), 1)
    spare = jnp.zeros((LANES - ROWS, STATE), F32)
    reads = [
        jnp.transpose(jnp.concatenate([read_ref[:, g * STATE:(g + 1) * STATE], spare], axis=0))
        for g in range(groups)
    ]
    sums = []
    for g in range(groups):
        total = jnp.zeros(lane.shape, F32)
        for j in range(ROWS):
            write = write_ref[j:j + 1, g * STATE:(g + 1) * STATE]
            fresh = []
            for h in range(g * per_group, (g + 1) * per_group):
                column = drive_t[h * HEAD_DIM:(h + 1) * HEAD_DIM, j:j + 1]
                block = decay_ref[j, h:h + 1, :] * prior_ref[0, j, h] + column * write
                fresh_ref[0, j, h] = block
                fresh.append(block)
            product = jnp.dot(
                jnp.concatenate(fresh, axis=0), reads[g],
                precision=lax.Precision.HIGHEST, preferred_element_type=F32,
            )
            total = jnp.where(lane == j, product, total)
        sums.append(total)
    readout = jnp.transpose(jnp.concatenate(sums, axis=0))[:ROWS]
    gated = (readout + skip_ref[...]) * gate_ref[...]
    squares = jnp.sum(gated * gated, axis=1, keepdims=True)
    inner = gated.shape[1]
    gated_ref[:, :inner] = gated * gain_ref[...]
    gated_ref[:, inner:] = split_sum(squares)


def output_kernel(
    n_dp, n_tp, rows, share, inner, layer, gated_ref, weight_ref, stream_ref, out_ref,
    weight_buf, mine_buf, gather_buf, part_buf, sum_buf, row_buf, load_sem,
    dp_send, dp_recv, rs_send, rs_recv, ag_send, ag_recv,
):
    dp, tp = lax.axis_index("dp"), lax.axis_index("tp")
    local = weight_ref.shape[1]
    width = weight_ref.shape[2]
    load = pltpu.make_async_copy(weight_ref.at[layer], weight_buf, load_sem.at[0])
    load.start()
    greet((("dp", n_dp), ("tp", n_tp)))
    mine_buf[...] = gated_ref[...].astype(BF16)
    gathers = []
    for k in range(1, n_dp):
        copy = remote(
            mine_buf, gather_buf.at[k - 1], dp_send.at[k - 1], dp_recv.at[k - 1], "dp",
            lax.rem(dp + k, n_dp),
        )
        copy.start()
        gathers.append(copy)

    per_dp = rows // share

    def product(block, owner):
        part = jnp.dot(block[:, :local], weight_buf[...], preferred_element_type=F32)
        for s in range(per_dp):
            slot = owner * per_dp + s
            part_buf[slot, :, :width] = part[s * share:(s + 1) * share].astype(BF16)
            part_buf[slot, :, width:] = block[s * share:(s + 1) * share, local:]

    load.wait()
    product(mine_buf[...], dp)
    for k in range(1, n_dp):
        gathers[k - 1].wait_recv()
        product(gather_buf[k - 1], lax.rem(dp + n_dp - k, n_dp))
    scatters = []
    for k in range(1, n_tp):
        peer = lax.rem(tp + k, n_tp)
        copy = remote(
            part_buf.at[peer], sum_buf.at[k - 1], rs_send.at[k - 1], rs_recv.at[k - 1], "tp", peer
        )
        copy.start()
        scatters.append(copy)
    total = part_buf[tp].astype(F32)
    for k in range(1, n_tp):
        scatters[k - 1].wait_recv()
        total = total + sum_buf[k - 1].astype(F32)
    squares = total[:, width:width + 1] + total[:, width + 1:width + 2]
    update = total[:, :width] * lax.rsqrt(squares / inner + EPS)
    row_buf[tp] = (stream_ref[tp].astype(F32) + update).astype(BF16)
    spreads = []
    for k in range(1, n_tp):
        copy = remote(
            row_buf.at[tp], row_buf.at[tp], ag_send.at[k - 1], ag_recv.at[k - 1], "tp",
            lax.rem(tp + k, n_tp),
        )
        copy.start()
        spreads.append(copy)
    out_ref[tp] = row_buf[tp]
    for k in range(1, n_tp):
        source = lax.rem(tp + n_tp - k, n_tp)
        remote(
            row_buf.at[source], row_buf.at[source], ag_send.at[k - 1], ag_recv.at[k - 1], "tp", source
        ).wait_recv()
        out_ref[source] = row_buf[source]
    for copy in gathers + scatters + spreads:
        copy.wait_send()


def whole(shape):
    return pl.BlockSpec(shape, lambda i: (0,) * len(shape))


def of_layer(shape, layer):
    return pl.BlockSpec((1,) + shape[1:], lambda i: (layer,) + (0,) * (len(shape) - 1))


def project(layer, n_dp, stream, gain, gate, inputs, coupling, steps):
    batch, width = stream.shape
    rows = batch // n_dp
    step_lanes = -(-steps.shape[1] // LANES) * LANES
    columns = gate.shape[2] + inputs.shape[2] + coupling.shape[1] + step_lanes
    return pl.pallas_call(
        functools.partial(project_kernel, n_dp, rows, width * n_dp, layer),
        grid=(1,),
        out_shape=jax.ShapeDtypeStruct((rows, columns), F32),
        in_specs=[
            whole(stream.shape),
            whole(gain.shape),
            pl.BlockSpec(memory_space=pl.ANY),
            pl.BlockSpec(memory_space=pl.ANY),
            pl.BlockSpec(memory_space=pl.ANY),
            of_layer(steps.shape, layer),
        ],
        out_specs=whole((rows, columns)),
        scratch_shapes=[
            pltpu.VMEM(gate.shape[1:], BF16),
            pltpu.VMEM(inputs.shape[1:], BF16),
            pltpu.VMEM(coupling.shape, BF16),
            pltpu.VMEM((n_dp, rows, columns + LANES), BF16),
            pltpu.VMEM((n_dp - 1, rows, columns + LANES), BF16),
            pltpu.SemaphoreType.DMA((3,)),
            pltpu.SemaphoreType.DMA((n_dp - 1,)),
            pltpu.SemaphoreType.DMA((n_dp - 1,)),
        ],
        compiler_params=pltpu.CompilerParams(
            collective_id=2 * layer, has_side_effects=True, vmem_limit_bytes=VMEM_LIMIT
        ),
    )(stream, gain, gate, inputs, coupling, steps)


def advance(layer, per_group, drive, decay, write, read, skip, gate, gain, recurrent, held):
    count, inner = drive.shape
    heads = recurrent.shape[2]

    def strip(width):
        return pl.BlockSpec((ROWS, width), lambda i: (i, 0))

    state_spec = pl.BlockSpec(
        (1, ROWS) + recurrent.shape[2:], lambda i: (layer, i, 0, 0, 0)
    )
    in_specs = [
        strip(inner),
        pl.BlockSpec((ROWS, heads, LANES), lambda i: (i, 0, 0)),
        strip(write.shape[1]),
        strip(read.shape[1]),
        strip(inner),
        strip(inner),
        whole(gain.shape),
        state_spec,
    ]
    operands = [drive, decay, write, read, skip, gate, gain, recurrent]
    aliases = {}
    if held is not None:
        aliases = {len(operands): 0}
        operands.append(held)
        in_specs.append(pl.BlockSpec(memory_space=pl.ANY))
    return pl.pallas_call(
        functools.partial(state_kernel, heads, per_group),
        grid=(count // ROWS,),
        out_shape=(
            jax.ShapeDtypeStruct(recurrent.shape, F32),
            jax.ShapeDtypeStruct((count, inner + LANES), F32),
        ),
        in_specs=in_specs,
        out_specs=(state_spec, strip(inner + LANES)),
        input_output_aliases=aliases,
        compiler_params=pltpu.CompilerParams(vmem_limit_bytes=VMEM_LIMIT),
    )(*operands)


def output(layer, n_dp, n_tp, gated, weight, stream):
    rows = gated.shape[0]
    share, width = stream.shape[1:]
    return pl.pallas_call(
        functools.partial(output_kernel, n_dp, n_tp, rows, share, weight.shape[1] * n_tp, layer),
        grid=(1,),
        out_shape=jax.ShapeDtypeStruct(stream.shape, BF16),
        in_specs=[
            whole(gated.shape), pl.BlockSpec(memory_space=pl.ANY), whole(stream.shape)
        ],
        out_specs=whole(stream.shape),
        scratch_shapes=[
            pltpu.VMEM(weight.shape[1:], BF16),
            pltpu.VMEM(gated.shape, BF16),
            pltpu.VMEM((n_dp - 1,) + gated.shape, BF16),
            pltpu.VMEM((n_tp, share, width + LANES), BF16),
            pltpu.VMEM((n_tp - 1, share, width + LANES), BF16),
            pltpu.VMEM(stream.shape, BF16),
            pltpu.SemaphoreType.DMA((1,)),
            pltpu.SemaphoreType.DMA((n_dp - 1,)),
            pltpu.SemaphoreType.DMA((n_dp - 1,)),
            pltpu.SemaphoreType.DMA((n_tp - 1,)),
            pltpu.SemaphoreType.DMA((n_tp - 1,)),
            pltpu.SemaphoreType.DMA((n_tp - 1,)),
            pltpu.SemaphoreType.DMA((n_tp - 1,)),
        ],
        compiler_params=pltpu.CompilerParams(
            collective_id=2 * layer + 1, has_side_effects=True, vmem_limit_bytes=VMEM_LIMIT
        ),
    )(gated, weight, stream)


def on_device(
    hidden,
    lengths,
    norm_gain,
    gate_proj,
    input_proj,
    coupling_proj,
    step_proj,
    input_taps,
    coupling_taps,
    step_bias,
    decay_log,
    skip_gain,
    span_bias,
    mix_gain,
    out_proj,
    recurrent,
    input_history,
    coupling_history,
):
    n_dp, n_tp = lax.axis_size("dp"), lax.axis_size("tp")
    batch, width = hidden.shape
    share = batch // n_tp
    rows, heads = recurrent.shape[1:3]
    inner = gate_proj.shape[2]
    groups = coupling_proj.shape[3] // STATE
    per_group = heads // groups
    half = groups * STATE
    steps_t = jnp.swapaxes(step_proj, 1, 2)
    span_index = (lengths - 1) // SPAN_LEN
    onehot = (span_index[:, None] == jnp.arange(SPANS, dtype=jnp.int32)[None, :]).astype(F32)
    stream = hidden.reshape(n_tp, share, width)
    states = None
    inputs_next, couplings_next = [], []
    for l in range(LAYERS):
        coupling = coupling_proj[l].reshape(width, 2 * half)
        sums = project(
            l, n_dp, stream.reshape(batch, width), norm_gain[l:l + 1], gate_proj, input_proj,
            coupling, steps_t,
        )
        gate_in = sums[:, :inner].astype(BF16)
        input_in = sums[:, inner:2 * inner].astype(BF16)
        coupling_in = sums[:, 2 * inner:2 * inner + 2 * half].astype(BF16).reshape(rows, 2, half)
        step_in = head_slice(sums[:, 2 * inner + 2 * half:][:, :step_proj.shape[2]], heads)
        step_in = step_in.astype(BF16)
        input_window = jnp.concatenate([input_history[l], input_in[:, None, :]], axis=1)
        coupling_window = jnp.concatenate([coupling_history[l], coupling_in[:, None]], axis=1)
        inputs_next.append(input_window[:, 1:])
        couplings_next.append(coupling_window[:, 1:])
        input_act = jax.nn.silu(jnp.sum(input_window.astype(F32) * input_taps[l][None], axis=1))
        coupling_act = jax.nn.silu(
            jnp.sum(coupling_window.astype(F32) * coupling_taps[l][None], axis=1)
        )
        span_term = jnp.sum(onehot[:, :, None] * head_slice(span_bias[l], heads)[None], axis=1)
        step_size = jax.nn.softplus(
            step_in.astype(F32) + head_slice(step_bias[l], heads)[None] + span_term
        )
        decay = jnp.exp(-step_size * jnp.exp(head_slice(decay_log[l], heads))[None])
        heads_in = input_act.reshape(rows, heads, HEAD_DIM)
        drive = (step_size[:, :, None] * heads_in).reshape(rows, inner)
        skip = (head_slice(skip_gain[l], heads)[None, :, None] * heads_in).reshape(rows, inner)
        states, gated = advance(
            l,
            per_group,
            drive,
            jnp.broadcast_to(decay[:, :, None], (rows, heads, LANES)),
            coupling_act[:, 0],
            coupling_act[:, 1],
            skip,
            jax.nn.silu(gate_in.astype(F32)),
            mix_gain[l:l + 1],
            recurrent,
            states,
        )
        stream = output(l, n_dp, n_tp, gated, out_proj, stream)
    return (
        stream.reshape(batch, width),
        states,
        jnp.stack(inputs_next),
        jnp.stack(couplings_next),
    )


def solution(mesh):
    placed = (
        P(None, "dp"),
        P("dp"),
        P(None, "dp"),
        P(None, "dp", "tp"),
        P(None, "dp", "tp"),
        P(None, "dp", None, "tp"),
        P(None, "dp", None),
        P(None, None, "tp"),
        P(None, None, None, "tp"),
        P(),
        P(),
        P(),
        P(),
        P(None, "tp"),
        P(None, "tp", "dp"),
        P(None, "dp", "tp", None, None),
        P(None, "dp", None, "tp"),
        P(None, "dp", None, None, "tp"),
    )
    return jax.shard_map(
        on_device,
        mesh=mesh,
        in_specs=placed,
        out_specs=(
            P(None, "dp"),
            P(None, "dp", "tp", None, None),
            P(None, "dp", None, "tp"),
            P(None, "dp", None, None, "tp"),
        ),
        check_vma=False,
    )
```
